32 devices in a mesh: sp: 8 (over z, x), dp: 4 (over y, core).
Axes of the slice: x: 2, y: 2, z: 4, core: 2. Of those that a mesh axis runs over, the one named last changes fastest.
Arguments:
- tokens: bfloat16 [4, 4096, 4096], P('dp', 'sp'), may hold values from -6 to 6
- documents: int32 [4, 4096], P('dp', 'sp'), may hold values from 0 to 7, never falling along the last dimension, each value on 1 to 1024 neighbouring positions
- value_weight: bfloat16 [4096, 2048], P(('sp', 'dp')), may hold values from -0.09375 to 0.09375
- gate_weight: bfloat16 [4096, 2048], P(('sp', 'dp')), may hold values from -0.09375 to 0.09375
- conv_weight: bfloat16 [31, 2048], replicated, may hold values from -1 to 1
- norm_gain: float32 [2048], replicated, may hold values from 0.1 to 1.9
- norm_bias: float32 [2048], replicated, may hold values from -2 to 2
Outputs:
- activated: bfloat16 [4, 4096, 2048], P('dp', 'sp')
The draws below stay inside these ranges and needn't reach their ends.
Inputs may be any that keep to these rules, and one draw needn't show every extreme that they name: `documents`: document numbers never fall along a sequence, run from 0 to 7, and each document covers 1 to 1024 positions.
All inputs are finite; a program needn't handle non-finite values.
Results may differ from the reference program's by a relative error of at most 0.0064.
Values may be sent and summed in bfloat16 or wider, within the bound.
No kernel may reach another device: no remote copies, remote signals or barrier semaphores. Data moves between devices by JAX's collectives and lax.ppermute only.
A program may use at most 192 MiB of HBM per device.

```python
import math
import jax
import jax.numpy as jnp
import numpy as np
from jax import lax

D = 4096
DB = 2048
KERNEL = 31
DOCS = 8
LENGTH = 4096
BATCH = 4


def levels(key, extent, pieces, smallest, high):
    def one(position, blocks):
        heights = jax.random.uniform(jax.random.fold_in(jax.random.fold_in(key, 6), position), (blocks,), jnp.float32, smallest / len(pieces), high / len(pieces))
        return jnp.repeat(jnp.exp(heights), extent[position] // blocks).reshape((-1,) + (1,) * (len(extent) - position - 1))

    factor_of = one(*pieces[0])
    for cut in pieces[1:]:
        factor_of = factor_of * one(*cut)
    return factor_of


def length_profile(amount, total, most, lean):
    portions = [(1 << 20) // math.isqrt(standing ** lean) + 1 for standing in range(2, amount + 1)]
    surplus, given = total - most - (amount - 1), [1] * (amount - 1)
    while surplus > 0:
        candidates = [i for i in range(amount - 1) if given[i] < most]
        pool, budget = sum([portions[i] for i in candidates]), surplus
        for i in candidates:
            extra = min(most - given[i], max(1, budget * portions[i] // pool), surplus)
            given[i] = given[i] + extra
            surplus = surplus - extra
    return np.array([most] + given)


def uneven(stream_key, number_of, total, reach, lean):
    if number_of == 2:
        one = jax.random.randint(stream_key, (), max(1, total - reach), min(reach, total - 1) + 1)
        return jnp.stack([one, total - one])
    tallies = jnp.asarray(length_profile(number_of, total, reach, lean), jnp.int32)
    twos = (number_of - 1) // 2
    donor, sink = tallies[1:1 + 2 * twos:2], tallies[2:2 + 2 * twos:2]
    slack = jnp.minimum(donor - 1, reach - sink)
    shifted = jax.random.randint(jax.random.fold_in(stream_key, 1), (twos,), 0, 1 << 20) % (slack + 1)
    tallies = tallies.at[1:1 + 2 * twos:2].set(donor - shifted).at[2:2 + 2 * twos:2].set(sink + shifted)
    return tallies[jax.random.permutation(jax.random.fold_in(stream_key, 2), number_of)]


def bell_draw(stream_key, dims, scale, bound, cuts=(), dtype=jnp.bfloat16):
    factor_of = levels(stream_key, dims, cuts, -0.22, 0.18) if cuts else 1.0
    entries = jax.random.normal(stream_key, dims, jnp.float32) * scale * factor_of
    return jnp.minimum(jnp.maximum(entries, -bound), bound).astype(dtype)


def setup_inputs(seed: int = 0) -> dict:
    streams_of = jax.random.split(jax.random.key(seed), 8)
    tokens = bell_draw(streams_of[0], (BATCH, LENGTH, D), 1.0, 6.0, ((0, 4), (1, 8)))
    documents = jax.vmap(lambda own: jnp.searchsorted(jnp.cumsum(uneven(own, DOCS, LENGTH, LENGTH // 4, 1)), jnp.arange(LENGTH), side="right"))(jax.random.split(streams_of[1], BATCH)).reshape((BATCH, LENGTH)).astype(jnp.int32)
    value_weight = bell_draw(streams_of[2], (D, DB), D ** -0.5, 0.09375, ((0, 32),))
    gate_weight = bell_draw(streams_of[3], (D, DB), D ** -0.5, 0.09375, ((0, 32),))
    conv_weight = bell_draw(streams_of[4], (KERNEL, DB), KERNEL ** -0.5, 1.0)
    norm_gain = jnp.clip(1.0 + 0.18 * jax.random.normal(streams_of[5], (DB,), jnp.float32), 0.1, 1.9)
    norm_bias = bell_draw(streams_of[6], (DB,), 0.5, 2.0, (), jnp.float32)
    return dict(tokens=tokens, documents=documents, value_weight=value_weight, gate_weight=gate_weight, conv_weight=conv_weight, norm_gain=norm_gain, norm_bias=norm_bias)


def convolve(padded, padded_docs, taps, count):
    lead = taps.shape[0] - 1
    here = padded_docs[:, lead:lead + count]
    total = jnp.zeros((padded.shape[0], count, padded.shape[2]), jnp.float32)
    for lag in range(taps.shape[0]):
        begin = lead - lag
        moved = padded[:, begin:begin + count].astype(jnp.float32)
        keep = (padded_docs[:, begin:begin + count] == here)[:, :, None]
        total = total + jnp.where(keep, moved, 0.0) * taps[lag].astype(jnp.float32)
    return total

def finish(mixed, norm_gain, norm_bias):
    wide = mixed.astype(jnp.float32)
    center = wide - lax.optimization_barrier(jnp.mean(wide, axis=-1, keepdims=True))
    spread = lax.optimization_barrier(jnp.mean(center * center, axis=-1, keepdims=True))
    normed = center * lax.rsqrt(spread + 1e-06) * norm_gain + norm_bias
    return jax.nn.silu(normed).astype(jnp.bfloat16)

def reference(tokens, documents, value_weight, gate_weight, conv_weight, norm_gain, norm_bias):
    lead = KERNEL - 1

    def one_row(pair):
        rows, row_docs = pair
        value = jnp.dot(rows, value_weight, preferred_element_type=jnp.float32).astype(jnp.bfloat16)
        gate = jnp.dot(rows, gate_weight, preferred_element_type=jnp.float32).astype(jnp.bfloat16)
        value, gate = lax.optimization_barrier((value, gate))
        glu = (value.astype(jnp.float32) * jax.nn.sigmoid(gate.astype(jnp.float32))).astype(jnp.bfloat16)
        glu = lax.optimization_barrier(glu)
        padded = jnp.pad(glu[None], ((0, 0), (lead, 0), (0, 0)))
        padded_docs = jnp.pad(row_docs[None], ((0, 0), (lead, 0)), constant_values=-1)
        mixed = convolve(padded, padded_docs, conv_weight, rows.shape[0]).astype(jnp.bfloat16)
        mixed = lax.optimization_barrier(mixed)
        return finish(mixed, norm_gain, norm_bias)[0]
    return lax.map(one_row, (tokens, documents))
```

```python
import functools

import jax
import jax.numpy as jnp
from jax import lax
from jax.experimental import pallas as pl
from jax.experimental.pallas import tpu as pltpu
from jax.sharding import PartitionSpec as P

KERNEL = 31
HALO = 32
SUB = 256
ROWS = 64
ORDERS = ("zxy", "zyx", "xzy", "yzx")
FLAT = ("sp", "dp")


class Grid:
    def __init__(self, mesh):
        devices = mesh.devices
        place = [(d.coords[2], d.coords[0], d.coords[1], d.core_on_chip) for d in devices.flat]
        axes = [sorted({p[i] for p in place}) for i in range(4)]
        self.size = dict(zip("zxyc", map(len, axes)))
        self.place = [tuple(axes[i].index(p[i]) for i in range(4)) for p in place]
        self.flat = {p: i for i, p in enumerate(self.place)}
        self.dp = devices.shape[1]

    def route(self, axis):
        a, n = "zxyc".index(axis), self.size[axis]
        moved = []
        for i, p in enumerate(self.place):
            q = list(p)
            q[a] = (q[a] + 1) % n
            moved.append((i, self.flat[tuple(q)]))
        return moved

    def shift(self, block, axis):
        return lax.ppermute(block, FLAT, self.route(axis))

    def origin_table(self):
        return jnp.asarray(self.place, jnp.int32)

    def rows_of(self, here, key):
        s = self.size
        z, x, y, c = (
            (here[i] - key[i] + s[a]) % s[a] for i, a in enumerate("zxyc")
        )
        sp = z * s["x"] + x
        dp = y * s["c"] + c
        return sp * self.dp + dp


def moved_keys(keys, axis, by):
    a = "zxyc".index(axis)
    return [k[:a] + (k[a] + by,) + k[a + 1 :] for k in keys]


def gather(grid, unit, order):
    first, second, third = order
    blocks, keys, cur = [unit], [(0, 0, 0, 0)], unit
    for i in range(1, grid.size[first]):
        cur = grid.shift(cur, first)
        blocks.append(cur)
        keys += moved_keys(keys[:1], first, i)
    cur = jnp.concatenate(blocks, axis=0) if len(blocks) > 1 else unit
    groups = [(cur, keys)]
    for i in range(1, grid.size[second]):
        cur = grid.shift(cur, second)
        groups.append((cur, moved_keys(keys, second, i)))
    per = max(1, len(groups) // 2)
    merged = []
    for i in range(0, len(groups), per):
        part = groups[i : i + per]
        block = jnp.concatenate([g for g, _ in part], axis=0) if len(part) > 1 else part[0][0]
        merged.append((block, sum((k for _, k in part), [])))
    out = []
    for block, keys in merged:
        out.append((block, keys))
        cur = block
        for i in range(1, grid.size[third]):
            cur = grid.shift(cur, third)
            out.append((cur, moved_keys(keys, third, i)))
    both = []
    for block, keys in out:
        both.append((block, keys))
        cur = block
        for i in range(1, grid.size["c"]):
            cur = grid.shift(cur, "c")
            both.append((cur, moved_keys(keys, "c", i)))
    return both


def chunk_body(counts, unit_rows, table, steady, tok, age, taps, *rest):
    pieces = rest[: len(counts)]
    out, wide, glu, sem = rest[len(counts) :]
    width = out.shape[1]
    count = out.shape[0]
    subs = width // SUB

    def start(s, slot):
        n = 0
        for piece, many in zip(pieces, counts):
            for j in range(many):
                row = pl.multiple_of(table[n], unit_rows)
                pltpu.make_async_copy(
                    piece.at[pl.ds(j * unit_rows, unit_rows), pl.ds(s * 2 * SUB, 2 * SUB)],
                    wide.at[slot, pl.ds(row, unit_rows)],
                    sem.at[slot],
                ).start()
                n += 1

    start(0, 0)
    for s in range(subs):
        slot = s % 2
        if s + 1 < subs:
            start(s + 1, 1 - slot)
        pltpu.make_async_copy(wide.at[slot], wide.at[slot], sem.at[slot]).wait()
        both = jnp.dot(tok[...], wide[slot], preferred_element_type=jnp.float32)
        value = both[:, :SUB].astype(jnp.bfloat16).astype(jnp.float32)
        gate = both[:, SUB:].astype(jnp.bfloat16).astype(jnp.float32)
        glu[...] = (value * jax.nn.sigmoid(gate)).astype(jnp.bfloat16).astype(jnp.float32)

        for lane in range(SUB // 128):
            lanes = slice(lane * 128, lane * 128 + 128)
            olanes = slice(s * SUB + lane * 128, s * SUB + lane * 128 + 128)

            def conv(b, masked):
                base = pl.multiple_of(b * ROWS, ROWS)
                x = glu[pl.ds(base, ROWS + HALO), lanes]
                ages = age[pl.ds(base, ROWS), :] if masked else None
                total = jnp.zeros((ROWS, 128), jnp.float32)
                for r in range(8):
                    moved = x if r == 0 else pltpu.roll(x, r, 0)
                    for q in range(4):
                        lag = 8 * q + r
                        if lag >= KERNEL:
                            continue
                        term = moved[HALO - 8 * q : HALO - 8 * q + ROWS]
                        if masked and lag:
                            term = jnp.where(ages >= lag, term, 0.0)
                        total = total + term * taps[pl.ds(lag, 1), olanes]
                out[pl.ds(base, ROWS), olanes] = total.astype(jnp.bfloat16)

            def step(b, carry):
                calm = steady[b] != 0

                @pl.when(calm)
                def _():
                    conv(b, False)

                @pl.when(jnp.logical_not(calm))
                def _():
                    conv(b, True)

                return carry

            lax.fori_loop(0, count // ROWS, step, 0)


def chunk_call(table, steady, tok, age, taps, pieces, unit_rows, width):
    counts = tuple(p.shape[0] // unit_rows for p in pieces)
    rows = age.shape[0]
    depth = tok.shape[1]
    vmem = pl.BlockSpec(memory_space=pltpu.VMEM)
    smem = pl.BlockSpec(memory_space=pltpu.SMEM)
    hbm = pl.BlockSpec(memory_space=pltpu.HBM)
    return pl.pallas_call(
        functools.partial(chunk_body, counts, unit_rows),
        out_shape=jax.ShapeDtypeStruct((rows, width), jnp.bfloat16),
        in_specs=[smem, smem, vmem, vmem, vmem] + [hbm] * len(pieces),
        out_specs=vmem,
        scratch_shapes=[
            pltpu.VMEM((2, depth, 2 * SUB), jnp.bfloat16),
            pltpu.VMEM((rows + HALO, SUB), jnp.float32),
            pltpu.SemaphoreType.DMA((2,)),
        ],
        cost_estimate=pl.CostEstimate(
            flops=2 * tok.shape[0] * depth * 2 * width,
            bytes_accessed=depth * 2 * width * 2,
            transcendentals=tok.shape[0] * width,
        ),
        compiler_params=pltpu.CompilerParams(vmem_limit_bytes=40 << 20),
        name="project_convolve",
    )(table, steady, tok, age, taps, *pieces)


def finish_body(gain, bias, *rest):
    parts, out = rest[:-1], rest[-1]
    channels = out.shape[1]

    def step(b, carry):
        rows = pl.ds(pl.multiple_of(b * ROWS, ROWS), ROWS)
        wide = jnp.concatenate([p[rows, :].astype(jnp.float32) for p in parts], axis=1)
        center = wide - jnp.sum(wide, axis=1, keepdims=True) * (1.0 / channels)
        spread = jnp.sum(center * center, axis=1, keepdims=True) * (1.0 / channels)
        normed = center * lax.rsqrt(spread + 1e-06) * gain[...] + bias[...]
        out[rows, :] = (normed * jax.nn.sigmoid(normed)).astype(jnp.bfloat16)
        return carry

    lax.fori_loop(0, out.shape[0] // ROWS, step, 0)


def finish_call(parts, gain, bias):
    rows = parts[0].shape[0]
    channels = sum(p.shape[1] for p in parts)
    vmem = pl.BlockSpec(memory_space=pltpu.VMEM)
    return pl.pallas_call(
        finish_body,
        out_shape=jax.ShapeDtypeStruct((rows, channels), jnp.bfloat16),
        in_specs=[vmem] * (2 + len(parts)),
        out_specs=vmem,
        compiler_params=pltpu.CompilerParams(vmem_limit_bytes=24 << 20),
        name="norm_swish",
    )(gain, bias, *parts)


def interleaved(value_weight, gate_weight, begin, width):
    cols = []
    for s in range(begin, begin + width, SUB):
        cols += [value_weight[:, s : s + SUB], gate_weight[:, s : s + SUB]]
    return jnp.concatenate(cols, axis=1)


def per_device(grid, tokens, documents, value_weight, gate_weight, conv_weight, norm_gain, norm_bias):
    batch, count, depth = tokens.shape
    unit_rows, channels = value_weight.shape
    sp, dp = lax.axis_size("sp"), lax.axis_size("dp")
    along = [(i * dp + j, (i + 1) * dp + j) for i in range(sp - 1) for j in range(dp)]

    width = channels // len(ORDERS)
    chunks = []
    for n, order in enumerate(ORDERS):
        unit = interleaved(value_weight, gate_weight, n * width, width)
        chunks.append(gather(grid, unit, order))

    before = lax.ppermute(tokens[0, count - HALO :], FLAT, along)
    before_docs = lax.ppermute(documents[:, count - HALO :], FLAT, along)
    first_span = lax.axis_index("sp") == 0
    docs = jnp.concatenate([jnp.where(first_span, -1, before_docs), documents], axis=1)[0]
    here = docs[HALO:]
    age = sum(
        (docs[HALO - k : HALO - k + count] == here).astype(jnp.int32) for k in range(1, KERNEL)
    )
    steady = jnp.min(age.reshape(count // ROWS, ROWS), axis=1) >= KERNEL - 1
    age = jnp.broadcast_to(age[:, None], (count, 128))
    tok = jnp.concatenate([before, tokens[0]], axis=0)
    taps = jnp.pad(conv_weight.astype(jnp.float32), ((0, 1), (0, 0)))

    here = [lax.axis_index("sp") // grid.size["x"], lax.axis_index("sp") % grid.size["x"],
            lax.axis_index("dp") // grid.size["c"], lax.axis_index("dp") % grid.size["c"]]
    parts = []
    for n, pieces in enumerate(chunks):
        table = jnp.stack([grid.rows_of(here, k) for _, keys in pieces for k in keys]) * unit_rows
        parts.append(
            chunk_call(
                table.astype(jnp.int32), steady.astype(jnp.int32), tok, age,
                taps[:, n * width : (n + 1) * width],
                [b for b, _ in pieces], unit_rows, width,
            )
        )
    out = finish_call(parts, norm_gain[None], norm_bias[None])
    return out[None]


def solution(mesh):
    return jax.shard_map(
        functools.partial(per_device, Grid(mesh)),
        mesh=mesh,
        in_specs=(
            P("dp", "sp", None),
            P("dp", "sp"),
            P(("sp", "dp"), None),
            P(("sp", "dp"), None),
            P(),
            P(),
            P(),
        ),
        out_specs=P("dp", "sp", None),
        check_vma=False,
    )
```
